32 devices in a mesh: sp: 8 (over z, y), dp: 4 (over x, core).
Axes of the slice: x: 2, y: 2, z: 4, core: 2. Of those that a mesh axis runs over, the one named last changes fastest.
Arguments:
- queries: bfloat16 [4, 1024, 2048], P('dp', 'sp'), may hold values from -8 to 8
- keys: bfloat16 [4, 1024, 2048], P('dp', 'sp'), may hold values from -8 to 8
- values: bfloat16 [4, 1024, 2048], P('dp', 'sp'), may hold values from -6 to 6
- proj_weight: bfloat16 [2048, 2048], P('sp'), may hold values from -0.125 to 0.125
- residual: bfloat16 [4, 1024, 2048], P('dp', 'sp'), may hold values from -6 to 6
- norm_gain: float32 [2048], replicated, may hold values from 0.1 to 1.9
- route: int32 [4, 1024, 2], P('dp', 'sp'), may hold values from 0 to 7, all different within a row; in each aligned block of 128 rows (0 to 127, 128 to 255, ..., all dimensions but the last counted through in order) at most 64 rows name the same one
- route_weight: float32 [4, 1024, 2], P('dp', 'sp'), may hold values from 0.1 to 1
- w_gate: bfloat16 [8, 2048, 1024], P('sp'), may hold values from -0.125 to 0.125
- w_up: bfloat16 [8, 2048, 1024], P('sp'), may hold values from -0.125 to 0.125
- w_down: bfloat16 [8, 1024, 2048], P('sp'), may hold values from -0.1875 to 0.1875
Outputs:
- mixed: bfloat16 [4, 1024, 2048], P('dp', 'sp')
The draws below stay inside these ranges and needn't reach their ends.
Inputs may be any that keep to these rules, and one draw needn't show every extreme that they name: `route`: in the rows of one device no expert is named by more than 64 rows, a bound that some block reaches.
All inputs are finite; a program needn't handle non-finite values.
Results may differ from the reference program's by a relative error of at most 0.013.
Values may be sent and summed in bfloat16 or wider, within the bound.
A program may use at most 128 MiB of HBM per device.

```python
import math
import jax
import jax.numpy as jnp
import numpy as np
from jax import lax

D = 2048
HEADS = 16
HEAD_DIM = 128
FFE = 1024
SEQ_DEV = 128
EXPERTS = 8
LENGTH = 1024
SEQS = 4
CAP = 64
N_SP = 8
N_DP = 4


def head_plan(key):
    first, second, third = jax.random.split(jax.random.fold_in(key, 7), 3)
    direction = jnp.where(jax.random.bernoulli(first, 0.5, (HEADS, HEAD_DIM)), 1.0, -1.0).astype(jnp.float32)
    slow = jax.random.bernoulli(second, 0.5, (HEADS,))
    level = jnp.where(slow, -jnp.log(1.0 * LENGTH) - 1.5, -jnp.log(100.0))
    drift = jax.random.uniform(third, (SEQS, LENGTH // 64, HEADS), jnp.float32, -0.8, 0.8)
    drift = jnp.repeat(drift, 64, axis=1)
    return (direction, level[None, None, :] + drift)


def noise(key):
    sample = jnp.clip(jax.random.normal(key, (SEQS, LENGTH, HEADS, HEAD_DIM), jnp.float32), -6.0, 6.0)
    return sample


def draw_keys(key, part):
    direction, level = head_plan(key)
    sample = noise(jax.random.fold_in(key, 11)) + direction[None, None, :, :]
    return sample.reshape(SEQS, LENGTH, HEADS * HEAD_DIM).astype(jnp.bfloat16)


def draw_queries(key, part):
    direction, level = head_plan(key)
    factor = level / jnp.sqrt(1.0 * HEAD_DIM)
    sample = noise(jax.random.fold_in(key, 13)) + factor[..., None] * direction[None, None, :, :]
    return sample.reshape(SEQS, LENGTH, HEADS * HEAD_DIM).astype(jnp.bfloat16)


def shard_levels(own_key, extent, pieces, low, high):
    gain, own = 1.0, jax.random.fold_in(own_key, 6)
    for dim, blocks in pieces:
        heights = jnp.exp(jax.random.uniform(jax.random.fold_in(own, dim), (blocks,), jnp.float32, low / len(pieces), high / len(pieces)))
        gain = gain * jnp.repeat(heights, extent[dim] // blocks).reshape([-1 if axis == dim else 1 for axis in range(len(extent))])
    return gain


def assign_block(stream_key, own, number, rows, amount, top, most, lean):
    order = jax.random.permutation(stream_key, amount)
    packed, common = portions_of(amount, rows * top, most, lean, True), portions_of(amount, rows * top, most, lean, False)
    places = jnp.arange(amount)

    def named(sizes, offset_by):
        used = int((sizes > 0).sum())
        fixed = max(1, used // 4)
        passed = fixed + (places - fixed + offset_by * (used - fixed)) % max(1, amount - fixed)
        return jnp.zeros((amount,), jnp.int32).at[order[jnp.where(places < fixed, places, passed)]].set(jnp.asarray(sizes, jnp.int32))

    sizes = jnp.where(number % 4 == 0, named(packed, number // 4), named(common, number - number // 4 - 1))
    mixed = jax.random.permutation(jax.random.fold_in(own, 3), amount)
    giver, receiver = mixed[0:amount // 2 * 2:2], mixed[1:amount // 2 * 2:2]
    margin = jnp.minimum(sizes[giver] - 1, most - sizes[receiver]) // 2
    margin = jnp.where((giver == order[0]) | (receiver == order[0]) | (sizes[receiver] == 0), 0, jnp.maximum(margin, 0))
    passed = jax.random.randint(jax.random.fold_in(own, 4), (amount // 2,), 0, 1 << 20) % (margin + 1)
    sizes = sizes.at[giver].add(-passed).at[receiver].add(passed)
    items = jnp.searchsorted(jnp.cumsum(sizes), jnp.arange(rows * top), side="right").astype(jnp.int32)
    grid = items.reshape(top, rows).T
    grid = grid[jax.random.permutation(jax.random.fold_in(own, 1), rows)]
    offset_by = jax.random.randint(jax.random.fold_in(own, 2), (rows, 1), 0, top)
    return jnp.take_along_axis(grid, (jnp.arange(top)[None, :] + offset_by) % top, axis=1)


def portions_of(count, total, reach, skew, full):
    loads = [(1 << 20) // math.isqrt(standing ** skew) + 1 for standing in range(1, count + 1)]
    largest = reach if full else min(reach, max(-(-total // count), total * loads[0] // sum(loads)))
    least = 1 if total - largest >= count - 1 else 0
    holding, surplus = [largest] + [least] * (count - 1), total - largest - least * (count - 1)
    while surplus > 0:
        movable = [i for i in range(1, count) if holding[i] < largest] or [i for i in range(1, count) if holding[i] < reach]
        whole, budget = sum([loads[i] for i in movable]), surplus
        for i in movable:
            extra = min(reach - holding[i], max(1, budget * loads[i] // whole), surplus)
            holding[i] = holding[i] + extra
            surplus = surplus - extra
    return np.array(holding)


def bell_draw(rng, extent, spread, most, shards=(), held_as=jnp.bfloat16):
    drawn = spread * jax.random.normal(rng, extent, jnp.float32)
    if shards:
        drawn = drawn * shard_levels(rng, extent, shards, -0.22, 0.18)
    return jnp.clip(drawn, -most, most).astype(held_as)


def setup_inputs(seed: int = 0) -> dict:
    splits = jax.random.split(jax.random.key(seed), 12)
    queries = draw_queries(jax.random.fold_in(splits[11], 71), 0)
    keys = draw_keys(jax.random.fold_in(splits[11], 71), 0)
    values = bell_draw(splits[2], (SEQS, LENGTH, D), 1.0, 6.0, ((0, 4), (1, 8)))
    proj_weight = bell_draw(splits[3], (D, D), D ** -0.5, 0.125, ((0, 8),))
    residual = bell_draw(splits[4], (SEQS, LENGTH, D), 1.0, 6.0, ((0, 4), (1, 8)))
    norm_gain = jnp.clip(1.0 + 0.18 * jax.random.normal(splits[5], (D,), jnp.float32), 0.1, 1.9)
    route_keys = jax.random.split(jax.random.fold_in(splits[6], 1), SEQS * LENGTH // SEQ_DEV)
    route_turns = jax.random.permutation(jax.random.fold_in(splits[6], 3), SEQS * LENGTH // SEQ_DEV)
    route = jax.vmap(lambda own, number: assign_block(jax.random.fold_in(splits[6], 2), own, number, SEQ_DEV, EXPERTS, 2, CAP, 2))(route_keys, route_turns).reshape((SEQS, LENGTH, 2))
    route_weight = jnp.clip(0.1 + 0.9 * jax.random.uniform(splits[7], (SEQS, LENGTH, 2), jnp.float32) ** shard_levels(splits[7], (SEQS, LENGTH, 2), ((0, 4), (1, 8)), -0.2, 0.2), 0.1, 1.0)
    w_gate = bell_draw(splits[8], (EXPERTS, D, FFE), D ** -0.5, 0.125, ((0, 8),))
    w_up = bell_draw(splits[9], (EXPERTS, D, FFE), D ** -0.5, 0.125, ((0, 8),))
    w_down = bell_draw(splits[10], (EXPERTS, FFE, D), FFE ** -0.5, 0.1875, ((0, 8),))
    return {"queries": queries, "keys": keys, "values": values, "proj_weight": proj_weight, "residual": residual, "norm_gain": norm_gain, "route": route, "route_weight": route_weight, "w_gate": w_gate, "w_up": w_up, "w_down": w_down}


EPS = 1e-06

def one_head(args):
    query, key, value = args
    length = query.shape[0]
    scores = jnp.dot(query, key.T, preferred_element_type=jnp.float32) * HEAD_DIM ** (-0.5)
    position = jnp.arange(length)
    causal = position[None, :] < position[:, None]
    softer = jnp.where(causal, jax.nn.softplus(scores), 0.0)
    suffix = lax.cumsum(softer, axis=1, reverse=True)
    weight = jnp.exp(jnp.where(causal, scores - suffix, -jnp.inf)).astype(jnp.bfloat16)
    return jnp.dot(weight, value, preferred_element_type=jnp.float32).astype(jnp.bfloat16)

def by_heads(array):
    seqs, length, width = array.shape
    heads = width // HEAD_DIM
    return array.reshape(seqs, length, heads, HEAD_DIM).transpose(0, 2, 1, 3).reshape(seqs * heads, length, HEAD_DIM)

def reference(queries, keys, values, proj_weight, residual, norm_gain, route, route_weight, w_gate, w_up, w_down):
    seqs, length, width = queries.shape
    heads = width // HEAD_DIM
    attended = lax.map(one_head, (by_heads(queries), by_heads(keys), by_heads(values)))
    attended = attended.reshape(seqs, heads, length, HEAD_DIM).transpose(0, 2, 1, 3).reshape(seqs * length, width)
    projected = jnp.dot(attended, proj_weight, preferred_element_type=jnp.float32)
    stream = (residual.reshape(seqs * length, width).astype(jnp.float32) + projected).astype(jnp.bfloat16)
    stream_f = stream.astype(jnp.float32)
    normed = (stream_f * lax.rsqrt(lax.optimization_barrier(jnp.mean(stream_f * stream_f, axis=-1, keepdims=True)) + EPS) * norm_gain).astype(jnp.bfloat16)
    flat_route = route.reshape(seqs * length, 2)
    flat_weight = route_weight.reshape(seqs * length, 2)
    bound = CAP * N_SP * N_DP

    def per_expert(total, inputs):
        expert, gate_w, up_w, down_w = inputs
        named = flat_route == expert
        scale = lax.optimization_barrier(jnp.sum(jnp.where(named, flat_weight, 0.0), axis=1))
        used = jnp.any(named, axis=1)
        index = jnp.nonzero(used, size=bound, fill_value=0)[0]
        valid = jnp.arange(bound) < jnp.sum(used.astype(jnp.int32))
        rows = normed[index]
        gate = jnp.dot(rows, gate_w, preferred_element_type=jnp.float32)
        upper = jnp.dot(rows, up_w, preferred_element_type=jnp.float32)
        hidden = (jax.nn.silu(gate) * upper).astype(jnp.bfloat16)
        result = jnp.dot(hidden, down_w, preferred_element_type=jnp.float32).astype(jnp.bfloat16)
        addend = jnp.where(valid[:, None], scale[index][:, None] * result.astype(jnp.float32), 0.0)
        return (total.at[index].add(addend), None)
    experts = w_gate.shape[0]
    total, unused = lax.scan(per_expert, stream.astype(jnp.float32), (jnp.arange(experts).astype(jnp.int32), w_gate, w_up, w_down))
    return total.astype(jnp.bfloat16).reshape(seqs, length, width)
```

```python
import functools
import math

import jax
import jax.numpy as jnp
from jax import lax
from jax.experimental import pallas as pl
from jax.experimental.pallas import tpu as pltpu
from jax.sharding import PartitionSpec as P

HEADS = 16


EPS = 1e-06

MESH = pl.DeviceIdType.MESH


def attention_kernel(
    n, m, ny, q_ref, k_ref, v_ref, proj_ref, res_ref, gain_ref, stream_ref, normed_ref,
    qbuf, kbuf, vbuf, wbuf, osend, obuf,
    in_send, in_recv, o_send, o_recv, w_send, w_recv,
):
    me, dp = lax.axis_index("sp"), lax.axis_index("dp")
    nz = n // ny
    z, y = me // ny, lax.rem(me, ny)
    cores = 2
    nx = m // cores
    x, core = dp // cores, lax.rem(dp, cores)
    rows, width = q_ref.shape
    cols = width // n
    head = width // HEADS
    heads_here = cols // head
    wcols = wbuf.shape[3]

    def peer(sp, d):
        return {"sp": sp, "dp": d}

    barrier = pltpu.get_barrier_semaphore()
    for off in range(1, n):
        pl.semaphore_signal(barrier, inc=1, device_id=peer(lax.rem(me + off, n), dp), device_id_type=MESH)
    for off in range(1, m):
        pl.semaphore_signal(barrier, inc=1, device_id=peer(me, lax.rem(dp + off, m)), device_id_type=MESH)
    pl.semaphore_wait(barrier, n - 1 + m - 1)

    def my_cols(d):
        return pl.ds(pl.multiple_of(d * cols, cols), cols)

    def row_block(d):
        return pl.ds(pl.multiple_of(d * rows, rows), rows)

    trio = ((k_ref, kbuf), (q_ref, qbuf), (v_ref, vbuf))

    def in_copy(t, off):
        ref, buf = trio[t]
        to = lax.rem(me + off, n)
        return pltpu.make_async_remote_copy(
            src_ref=ref.at[:, my_cols(to)], dst_ref=buf.at[row_block(me), :],
            send_sem=in_send.at[t, off], recv_sem=in_recv.at[t, off],
            device_id=peer(to, dp), device_id_type=MESH,
        )

    def in_wait(t, off):
        ref, buf = trio[t]
        origin = lax.rem(me - off + n, n)
        pltpu.make_async_remote_copy(
            src_ref=ref.at[:, my_cols(me)], dst_ref=buf.at[row_block(origin), :],
            send_sem=in_send.at[t, off], recv_sem=in_recv.at[t, off],
            device_id=peer(origin, dp), device_id_type=MESH,
        ).wait_recv()

    for t in range(3):
        for off in range(1, n):
            in_copy(t, off).start()

    sent = []

    def w_start(cond, q, i, dev, own=False):
        slot = len(sent)
        source = proj_ref.at[:, pl.ds(pl.multiple_of(q * wcols, wcols), wcols)] if own else wbuf.at[q, i]
        copy = pltpu.make_async_remote_copy(
            src_ref=source, dst_ref=wbuf.at[q, i],
            send_sem=w_send.at[slot], recv_sem=w_recv.at[q, i],
            device_id=dev, device_id_type=MESH,
        )
        sent.append((cond, copy))
        if cond is None:
            copy.start()
        else:
            pl.when(cond)(copy.start)

    def w_wait(cond, q, i):
        copy = pltpu.make_async_remote_copy(
            src_ref=wbuf.at[q, i], dst_ref=wbuf.at[q, i],
            send_sem=w_send.at[0], recv_sem=w_recv.at[q, i],
            device_id=peer(me, lax.rem(dp + 1, m)), device_id_type=MESH,
        )
        if cond is None:
            copy.wait_recv()
        else:
            pl.when(cond)(copy.wait_recv)

    up, down = z + 1 < nz, z > 0
    above, below = jnp.minimum(z + 1, nz - 1) * ny + y, jnp.maximum(z - 1, 0) * ny + y
    other = x * cores + lax.rem(core + 1, cores)
    w_start(up, dp, me, peer(above, dp), True)
    w_start(down, dp, me, peer(below, dp), True)
    for o in range(1, ny):
        w_start(None, dp, me, peer(z * ny + lax.rem(y + o, ny), dp), True)

    for q in range(m):
        wbuf[q, me] = proj_ref[:, q * wcols : (q + 1) * wcols]
    for ref, buf in trio:
        buf[row_block(me), :] = ref[:, my_cols(me)]

    def across(cond, i):
        for o in range(1, nx):
            w_start(cond, dp, i, peer(me, lax.rem(x + o, nx) * cores + core), False)
        w_start(cond, dp, i, peer(me, other), False)

    def column(dz, upward):
        def run():
            far = z - dz if upward else z + dz
            cond = far >= 0 if upward else far < nz
            far = jnp.clip(far, 0, nz - 1)
            i = far * ny + y
            w_wait(cond, dp, i)
            more = jnp.logical_and(cond, up if upward else down)
            if dz < nz - 1:
                w_start(more, dp, i, peer(above if upward else below, dp))
            for o in range(1, ny):
                w_start(cond, dp, i, peer(z * ny + lax.rem(y + o, ny), dp))
            across(cond, i)
        return run

    def side(dz, upward, o):
        def run():
            far = z - dz if upward else z + dz
            cond = (far >= 0 if upward else far < nz) if dz else None
            far = jnp.clip(far, 0, nz - 1)
            i = far * ny + lax.rem(y + o, ny)
            w_wait(cond, dp, i)
            across(cond, i)
        return run

    def beyond(off, o):
        def run():
            i = lax.rem(me + off, n)
            q = lax.rem(x + o, nx) * cores + core
            w_wait(None, q, i)
            w_start(None, q, i, peer(me, other))
        return run

    tasks = [side(0, True, o) for o in range(1, ny)]
    for dz in range(1, nz):
        tasks += [column(dz, True), column(dz, False)]
        tasks += [side(dz, way, o) for o in range(1, ny) for way in (True, False)]
    late = [beyond(off, o) for off in range(1, n) for o in range(1, nx)]

    def o_copy(d):
        return pltpu.make_async_remote_copy(
            src_ref=osend.at[d], dst_ref=obuf.at[me],
            send_sem=o_send.at[d], recv_sem=o_recv.at[me],
            device_id=peer(d, dp), device_id_type=MESH,
        )

    for t in range(3):
        for off in range(1, n):
            in_wait(t, off)

    scale = 1.0 / math.sqrt(head)
    row_id = lax.broadcasted_iota(jnp.int32, (rows, rows), 0)
    col_id = lax.broadcasted_iota(jnp.int32, (rows, rows), 1)
    later = (row_id > col_id).astype(jnp.bfloat16)
    inside = col_id < row_id

    def attend(d):
        for h in range(heads_here):
            lanes = slice(h * head, (h + 1) * head)
            query = qbuf[d * rows : (d + 1) * rows, lanes]
            total = jnp.zeros((rows, head), jnp.float32)
            carry = jnp.zeros((rows, 1), jnp.float32)
            for b in range(d, -1, -1):
                block = slice(b * rows, (b + 1) * rows)
                score = lax.dot_general(
                    query, kbuf[block, lanes], (((1,), (1,)), ((), ())),
                    preferred_element_type=jnp.float32,
                ) * scale
                soft = jnp.maximum(score, 0.0) + jnp.log1p(jnp.exp(-jnp.abs(score)))
                log_sigmoid = score - soft
                if b == d:
                    soft = jnp.where(inside, soft, 0.0)
                high = soft.astype(jnp.bfloat16)
                low = (soft - high.astype(jnp.float32)).astype(jnp.bfloat16)
                suffix = jnp.dot(high, later, preferred_element_type=jnp.float32) + jnp.dot(
                    low, later, preferred_element_type=jnp.float32
                )
                weight = jnp.exp(log_sigmoid - suffix - carry)
                if b == d:
                    weight = jnp.where(inside, weight, 0.0)
                carry = carry + suffix[:, 0:1] + soft[:, 0:1]
                total = total + jnp.dot(
                    weight.astype(jnp.bfloat16), vbuf[block, lanes], preferred_element_type=jnp.float32
                )
            osend[d, :, lanes] = total.astype(jnp.bfloat16)

    done = 0
    for d in range(n):
        attend(d)

        @pl.when(me == d)
        def _():
            obuf[me] = osend[d]

        @pl.when(me != d)
        def _():
            o_copy(d).start()

        share = (d + 1) * len(tasks) // n
        for run in tasks[done:share]:
            run()
        done = share
    for run in late:
        run()
    for off in range(1, n):
        i = lax.rem(me + off, n)
        for x_off in range(nx):
            w_wait(None, lax.rem(x + x_off, nx) * cores + lax.rem(core + 1, cores), i)
    for off in range(1, n):
        origin = lax.rem(me - off + n, n)
        pltpu.make_async_remote_copy(
            src_ref=osend.at[0], dst_ref=obuf.at[origin],
            send_sem=o_send.at[0], recv_sem=o_recv.at[origin],
            device_id=peer(origin, dp), device_id_type=MESH,
        ).wait_recv()

    square = jnp.zeros((rows, 1), jnp.float32)
    attended = jnp.concatenate([obuf[i] for i in range(n)], axis=1)
    for q in range(m):
        part = slice(q * wcols, (q + 1) * wcols)
        weights = wbuf[q].reshape(width, wcols)
        acc = jnp.dot(attended, weights, preferred_element_type=jnp.float32)
        stream = (res_ref[:, part].astype(jnp.float32) + acc).astype(jnp.bfloat16)
        stream_ref[:, part] = stream
        stream = stream.astype(jnp.float32)
        square = square + jnp.sum(stream * stream, axis=1, keepdims=True)
    factor = lax.rsqrt(square / width + EPS)
    for q in range(m):
        part = slice(q * wcols, (q + 1) * wcols)
        normed_ref[:, part] = (
            stream_ref[:, part].astype(jnp.float32) * factor * gain_ref[:, part]
        ).astype(jnp.bfloat16)

    for t in range(3):
        for off in range(1, n):
            in_copy(t, off).wait_send()
    for d in range(n):
        @pl.when(me != d)
        def _():
            o_copy(d).wait_send()
    for cond, copy in sent:
        if cond is None:
            copy.wait_send()
        else:
            pl.when(cond)(copy.wait_send)


def attention(queries, keys, values, proj_weight, residual, norm_gain):
    n, m = lax.axis_size("sp"), lax.axis_size("dp")
    rows, width = queries.shape
    cols = width // n
    ny = 1 << ((n.bit_length() - 1) // 2)
    nz, nx = n // ny, m // 2
    copies = 1 + ny + 2 * nz * (ny + nx + 1) + (2 * nz) * ny * nx + n * nx
    bf16 = jnp.bfloat16
    vmem = pl.BlockSpec(memory_space=pltpu.VMEM)
    return pl.pallas_call(
        functools.partial(attention_kernel, n, m, ny),
        out_shape=[jax.ShapeDtypeStruct((rows, width), bf16)] * 2,
        in_specs=[vmem] * 6,
        out_specs=[vmem] * 2,
        scratch_shapes=[
            pltpu.VMEM((n * rows, cols), bf16),
            pltpu.VMEM((n * rows, cols), bf16),
            pltpu.VMEM((n * rows, cols), bf16),
            pltpu.VMEM((m, n, cols, width // m), bf16),
            pltpu.VMEM((n, rows, cols), bf16),
            pltpu.VMEM((n, rows, cols), bf16),
            pltpu.SemaphoreType.DMA((3, n)),
            pltpu.SemaphoreType.DMA((3, n)),
            pltpu.SemaphoreType.DMA((n,)),
            pltpu.SemaphoreType.DMA((n,)),
            pltpu.SemaphoreType.DMA((copies,)),
            pltpu.SemaphoreType.DMA((m, n)),
        ],
        compiler_params=pltpu.CompilerParams(
            collective_id=0, has_side_effects=True, vmem_limit_bytes=50 * 1024 * 1024
        ),
    )(queries, keys, values, proj_weight, residual, norm_gain.reshape(1, width))


def body(
    queries,
    keys,
    values,
    proj_weight,
    residual,
    norm_gain,
    route,
    route_weight,
    w_gate,
    w_up,
    w_down,
):
    seq_span = lax.axis_size("sp")
    rows = queries.shape[1]
    width = queries.shape[2]
    stream, normed = attention(
        queries[0], keys[0], values[0], proj_weight, residual[0], norm_gain
    )
    stream_f = stream.astype(jnp.float32)
    capacity = 4 * rows // seq_span
    chosen = route[0].reshape(rows * 2)
    one_hot = (chosen[:, None] == jnp.arange(seq_span, dtype=jnp.int32)[None, :]).astype(jnp.int32)
    earlier = jnp.cumsum(one_hot, axis=0) - one_hot
    slot = jnp.sum(earlier * one_hot, axis=1)
    target = chosen * capacity + slot
    source_row = jnp.arange(rows * 2, dtype=jnp.int32) // 2
    slot_source = jnp.zeros((seq_span * capacity,), jnp.int32).at[target].set(source_row)
    slot_used = jnp.zeros((seq_span * capacity,), jnp.bool_).at[target].set(True)
    outgoing = jnp.where(slot_used[:, None], normed[slot_source], jnp.zeros((), jnp.bfloat16))
    outgoing = outgoing.reshape(seq_span, capacity, width)
    arrived = lax.all_to_all(outgoing, "sp", split_axis=0, concat_axis=0, tiled=True)
    senders, slots, features = arrived.shape
    flat = arrived.reshape(senders * slots, features)
    gate = jnp.dot(flat, w_gate[0], preferred_element_type=jnp.float32)
    upper = jnp.dot(flat, w_up[0], preferred_element_type=jnp.float32)
    hidden = (jax.nn.silu(gate) * upper).astype(jnp.bfloat16)
    result = jnp.dot(hidden, w_down[0], preferred_element_type=jnp.float32).astype(jnp.bfloat16)
    returned = lax.all_to_all(
        result.reshape(senders, slots, features), "sp", split_axis=0, concat_axis=0, tiled=True
    )
    picked = returned.reshape(seq_span * capacity, width)[target].reshape(rows, 2, width)
    mixed = stream_f + jnp.sum(route_weight[0][:, :, None] * picked.astype(jnp.float32), axis=1)
    return mixed.astype(jnp.bfloat16)[None]


def solution(mesh):
    return jax.shard_map(
        body,
        mesh=mesh,
        in_specs=(
            P("dp", "sp", None),
            P("dp", "sp", None),
            P("dp", "sp", None),
            P("sp", None),
            P("dp", "sp", None),
            P(),
            P("dp", "sp", None),
            P("dp", "sp", None),
            P("sp", None, None),
            P("sp", None, None),
            P("sp", None, None),
        ),
        out_specs=P("dp", "sp", None),
        check_vma=False,
    )
```

```python
import functools
import math

import jax
import jax.numpy as jnp
from jax import lax
from jax.experimental import pallas as pl
from jax.experimental.pallas import tpu as pltpu
from jax.sharding import PartitionSpec as P

HEADS = 16


EPS = 1e-06

MESH = pl.DeviceIdType.MESH


def attention_kernel(
    n, m, ny, q_ref, k_ref, v_ref, proj_ref, res_ref, gain_ref, stream_ref, normed_ref,
    qbuf, kbuf, vbuf, wbuf, osend, obuf,
    in_send, in_recv, o_send, o_recv, w_send, w_recv,
):
    me, dp = lax.axis_index("sp"), lax.axis_index("dp")
    nz = n // ny
    z, y = me // ny, lax.rem(me, ny)
    cores = 2
    nx = m // cores
    x, core = dp // cores, lax.rem(dp, cores)
    rows, width = q_ref.shape
    cols = width // n
    head = width // HEADS
    heads_here = cols // head
    wcols = wbuf.shape[3]

    def peer(sp, d):
        return {"sp": sp, "dp": d}

    barrier = pltpu.get_barrier_semaphore()
    for off in range(1, n):
        pl.semaphore_signal(barrier, inc=1, device_id=peer(lax.rem(me + off, n), dp), device_id_type=MESH)
    for off in range(1, m):
        pl.semaphore_signal(barrier, inc=1, device_id=peer(me, lax.rem(dp + off, m)), device_id_type=MESH)
    pl.semaphore_wait(barrier, n - 1 + m - 1)

    def my_cols(d):
        return pl.ds(pl.multiple_of(d * cols, cols), cols)

    def row_block(d):
        return pl.ds(pl.multiple_of(d * rows, rows), rows)

    trio = ((k_ref, kbuf), (q_ref, qbuf), (v_ref, vbuf))

    def in_copy(t, off):
        ref, buf = trio[t]
        to = lax.rem(me + off, n)
        return pltpu.make_async_remote_copy(
            src_ref=ref.at[:, my_cols(to)], dst_ref=buf.at[row_block(me), :],
            send_sem=in_send.at[t, off], recv_sem=in_recv.at[t, off],
            device_id=peer(to, dp), device_id_type=MESH,
        )

    def in_wait(t, off):
        ref, buf = trio[t]
        origin = lax.rem(me - off + n, n)
        pltpu.make_async_remote_copy(
            src_ref=ref.at[:, my_cols(me)], dst_ref=buf.at[row_block(origin), :],
            send_sem=in_send.at[t, off], recv_sem=in_recv.at[t, off],
            device_id=peer(origin, dp), device_id_type=MESH,
        ).wait_recv()

    for t in range(3):
        for off in range(1, n):
            in_copy(t, off).start()

    sent = []

    def w_start(cond, q, i, dev, own=False):
        slot = len(sent)
        source = proj_ref.at[:, pl.ds(pl.multiple_of(q * wcols, wcols), wcols)] if own else wbuf.at[q, i]
        copy = pltpu.make_async_remote_copy(
            src_ref=source, dst_ref=wbuf.at[q, i],
            send_sem=w_send.at[slot], recv_sem=w_recv.at[q, i],
            device_id=dev, device_id_type=MESH,
        )
        sent.append((cond, copy))
        if cond is None:
            copy.start()
        else:
            pl.when(cond)(copy.start)

    def w_wait(cond, q, i):
        copy = pltpu.make_async_remote_copy(
            src_ref=wbuf.at[q, i], dst_ref=wbuf.at[q, i],
            send_sem=w_send.at[0], recv_sem=w_recv.at[q, i],
            device_id=peer(me, lax.rem(dp + 1, m)), device_id_type=MESH,
        )
        if cond is None:
            copy.wait_recv()
        else:
            pl.when(cond)(copy.wait_recv)

    up, down = z + 1 < nz, z > 0
    above, below = jnp.minimum(z + 1, nz - 1) * ny + y, jnp.maximum(z - 1, 0) * ny + y
    other = x * cores + lax.rem(core + 1, cores)
    w_start(up, dp, me, peer(above, dp), True)
    w_start(down, dp, me, peer(below, dp), True)
    for o in range(1, ny):
        w_start(None, dp, me, peer(z * ny + lax.rem(y + o, ny), dp), True)

    for q in range(m):
        wbuf[q, me] = proj_ref[:, q * wcols : (q + 1) * wcols]
    for ref, buf in trio:
        buf[row_block(me), :] = ref[:, my_cols(me)]

    def across(cond, i):
        for o in range(1, nx):
            w_start(cond, dp, i, peer(me, lax.rem(x + o, nx) * cores + core), False)
        w_start(cond, dp, i, peer(me, other), False)

    def column(dz, upward):
        def run():
            far = z - dz if upward else z + dz
            cond = far >= 0 if upward else far < nz
            far = jnp.clip(far, 0, nz - 1)
            i = far * ny + y
            w_wait(cond, dp, i)
            more = jnp.logical_and(cond, up if upward else down)
            if dz < nz - 1:
                w_start(more, dp, i, peer(above if upward else below, dp))
            for o in range(1, ny):
                w_start(cond, dp, i, peer(z * ny + lax.rem(y + o, ny), dp))
            across(cond, i)
        return run

    def side(dz, upward, o):
        def run():
            far = z - dz if upward else z + dz
            cond = (far >= 0 if upward else far < nz) if dz else None
            far = jnp.clip(far, 0, nz - 1)
            i = far * ny + lax.rem(y + o, ny)
            w_wait(cond, dp, i)
            across(cond, i)
        return run

    def beyond(off, o):
        def run():
            i = lax.rem(me + off, n)
            q = lax.rem(x + o, nx) * cores + core
            w_wait(None, q, i)
            w_start(None, q, i, peer(me, other))
        return run

    tasks = [side(0, True, o) for o in range(1, ny)]
    for dz in range(1, nz):
        tasks += [column(dz, True), column(dz, False)]
        tasks += [side(dz, way, o) for o in range(1, ny) for way in (True, False)]
    late = [beyond(off, o) for off in range(1, n) for o in range(1, nx)]

    def o_copy(d):
        return pltpu.make_async_remote_copy(
            src_ref=osend.at[d], dst_ref=obuf.at[me],
            send_sem=o_send.at[d], recv_sem=o_recv.at[me],
            device_id=peer(d, dp), device_id_type=MESH,
        )

    for t in range(3):
        for off in range(1, n):
            in_wait(t, off)

    scale = 1.0 / math.sqrt(head)
    row_id = lax.broadcasted_iota(jnp.int32, (rows, rows), 0)
    col_id = lax.broadcasted_iota(jnp.int32, (rows, rows), 1)
    later = (row_id > col_id).astype(jnp.bfloat16)
    inside = col_id < row_id

    def attend(d):
        for h in range(heads_here):
            lanes = slice(h * head, (h + 1) * head)
            query = qbuf[d * rows : (d + 1) * rows, lanes]
            total = jnp.zeros((rows, head), jnp.float32)
            carry = jnp.zeros((rows, 1), jnp.float32)
            for b in range(d, -1, -1):
                block = slice(b * rows, (b + 1) * rows)
                score = lax.dot_general(
                    query, kbuf[block, lanes], (((1,), (1,)), ((), ())),
                    preferred_element_type=jnp.float32,
                ) * scale
                soft = jnp.maximum(score, 0.0) + jnp.log1p(jnp.exp(-jnp.abs(score)))
                log_sigmoid = score - soft
                if b == d:
                    soft = jnp.where(inside, soft, 0.0)
                high = soft.astype(jnp.bfloat16)
                low = (soft - high.astype(jnp.float32)).astype(jnp.bfloat16)
                suffix = jnp.dot(high, later, preferred_element_type=jnp.float32) + jnp.dot(
                    low, later, preferred_element_type=jnp.float32
                )
                weight = jnp.exp(log_sigmoid - suffix - carry)
                if b == d:
                    weight = jnp.where(inside, weight, 0.0)
                carry = carry + suffix[:, 0:1] + soft[:, 0:1]
                total = total + jnp.dot(
                    weight.astype(jnp.bfloat16), vbuf[block, lanes], preferred_element_type=jnp.float32
                )
            osend[d, :, lanes] = total.astype(jnp.bfloat16)

    done = 0
    for d in range(n):
        attend(d)

        @pl.when(me == d)
        def _():
            obuf[me] = osend[d]

        @pl.when(me != d)
        def _():
            o_copy(d).start()

        share = (d + 1) * len(tasks) // n
        for run in tasks[done:share]:
            run()
        done = share
    for run in late:
        run()
    for off in range(1, n):
        i = lax.rem(me + off, n)
        for x_off in range(nx):
            w_wait(None, lax.rem(x + x_off, nx) * cores + lax.rem(core + 1, cores), i)
    for off in range(1, n):
        origin = lax.rem(me - off + n, n)
        pltpu.make_async_remote_copy(
            src_ref=osend.at[0], dst_ref=obuf.at[origin],
            send_sem=o_send.at[0], recv_sem=o_recv.at[origin],
            device_id=peer(origin, dp), device_id_type=MESH,
        ).wait_recv()

    square = jnp.zeros((rows, 1), jnp.float32)
    attended = jnp.concatenate([obuf[i] for i in range(n)], axis=1)
    for q in range(m):
        part = slice(q * wcols, (q + 1) * wcols)
        weights = wbuf[q].reshape(width, wcols)
        acc = jnp.dot(attended, weights, preferred_element_type=jnp.float32)
        stream = (res_ref[:, part].astype(jnp.float32) + acc).astype(jnp.bfloat16)
        stream_ref[:, part] = stream
        stream = stream.astype(jnp.float32)
        square = square + jnp.sum(stream * stream, axis=1, keepdims=True)
    factor = lax.rsqrt(square / width + EPS)
    for q in range(m):
        part = slice(q * wcols, (q + 1) * wcols)
        normed_ref[:, part] = (
            stream_ref[:, part].astype(jnp.float32) * factor * gain_ref[:, part]
        ).astype(jnp.bfloat16)

    for t in range(3):
        for off in range(1, n):
            in_copy(t, off).wait_send()
    for d in range(n):
        @pl.when(me != d)
        def _():
            o_copy(d).wait_send()
    for cond, copy in sent:
        if cond is None:
            copy.wait_send()
        else:
            pl.when(cond)(copy.wait_send)


def attention(queries, keys, values, proj_weight, residual, norm_gain):
    n, m = lax.axis_size("sp"), lax.axis_size("dp")
    rows, width = queries.shape
    cols = width // n
    ny = 1 << ((n.bit_length() - 1) // 2)
    nz, nx = n // ny, m // 2
    copies = 1 + ny + 2 * nz * (ny + nx + 1) + (2 * nz) * ny * nx + n * nx
    bf16 = jnp.bfloat16
    vmem = pl.BlockSpec(memory_space=pltpu.VMEM)
    return pl.pallas_call(
        functools.partial(attention_kernel, n, m, ny),
        out_shape=[jax.ShapeDtypeStruct((rows, width), bf16)] * 2,
        in_specs=[vmem] * 6,
        out_specs=[vmem] * 2,
        scratch_shapes=[
            pltpu.VMEM((n * rows, cols), bf16),
            pltpu.VMEM((n * rows, cols), bf16),
            pltpu.VMEM((n * rows, cols), bf16),
            pltpu.VMEM((m, n, cols, width // m), bf16),
            pltpu.VMEM((n, rows, cols), bf16),
            pltpu.VMEM((n, rows, cols), bf16),
            pltpu.SemaphoreType.DMA((3, n)),
            pltpu.SemaphoreType.DMA((3, n)),
            pltpu.SemaphoreType.DMA((n,)),
            pltpu.SemaphoreType.DMA((n,)),
            pltpu.SemaphoreType.DMA((copies,)),
            pltpu.SemaphoreType.DMA((m, n)),
        ],
        compiler_params=pltpu.CompilerParams(
            collective_id=0, has_side_effects=True, vmem_limit_bytes=50 * 1024 * 1024
        ),
    )(queries, keys, values, proj_weight, residual, norm_gain.reshape(1, width))


def flipped(number, off, n):
    result = number
    bit = 1
    while bit < n:
        result = result + bit * lax.rem(off // bit, 2) * (1 - 2 * lax.rem(number // bit, 2))
        bit *= 2
    return result


def expert_kernel(
    n, normed_ref, stream_ref, target_ref, flat_ref, share_ref, gate_hbm, up_hbm, down_hbm, out_ref,
    gate_ref, up_ref, down_ref, outgoing, inbox, outbox, back, total,
    load_sem, there_send, there_recv, back_send, back_recv,
):
    me, dp = lax.axis_index("sp"), lax.axis_index("dp")
    rows, width = normed_ref.shape
    capacity = inbox.shape[1]
    pairs = n // 2

    loads = [
        pltpu.make_async_copy(gate_hbm.at[0], gate_ref, load_sem.at[0]),
        pltpu.make_async_copy(up_hbm.at[0], up_ref, load_sem.at[1]),
        pltpu.make_async_copy(down_hbm.at[0], down_ref, load_sem.at[2]),
    ]
    for load in loads:
        load.start()

    barrier = pltpu.get_barrier_semaphore()
    for off in range(1, n):
        pl.semaphore_signal(
            barrier, inc=1, device_id={"sp": lax.rem(me + off, n), "dp": dp}, device_id_type=MESH
        )

    def gathered(expert):
        slot = lax.broadcasted_iota(jnp.int32, (capacity, rows), 0) + expert * capacity
        chosen = jnp.logical_or(flat_ref[0:1, :] == slot, flat_ref[1:2, :] == slot)
        return jnp.dot(
            chosen.astype(jnp.bfloat16), normed_ref[...], preferred_element_type=jnp.float32
        ).astype(jnp.bfloat16)

    def there(off):
        return pltpu.make_async_remote_copy(
            src_ref=outgoing.at[off], dst_ref=inbox.at[off],
            send_sem=there_send.at[off], recv_sem=there_recv.at[off],
            device_id={"sp": flipped(me, off, n), "dp": dp}, device_id_type=MESH,
        )

    def home(off):
        return pltpu.make_async_remote_copy(
            src_ref=outbox.at[off], dst_ref=back.at[off],
            send_sem=back_send.at[off], recv_sem=back_recv.at[off],
            device_id={"sp": flipped(me, off, n), "dp": dp}, device_id_type=MESH,
        )

    pl.semaphore_wait(barrier, n - 1)

    @pl.loop(0, n)
    def _(step):
        pair = lax.rem(pairs - step // 2, pairs)
        off = pair * 2 + 1 - lax.rem(step, 2)
        block = gathered(flipped(me, off, n))

        @pl.when(off > 0)
        def _():
            outgoing[off] = block
            there(off).start()

        @pl.when(off == 0)
        def _():
            inbox[0] = block

    for load in loads:
        load.wait()

    hidden_width = gate_ref.shape[1]
    piece = min(512, hidden_width)

    @pl.loop(0, pairs)
    def _(step):
        pair = lax.rem(pairs - step, pairs)

        @pl.when(pair > 0)
        def _():
            there(pair * 2).wait_recv()

        there(pair * 2 + 1).wait_recv()
        arrived = inbox[pl.ds(pair * 2, 2)].reshape(2 * capacity, width)
        hidden = []
        for first in range(0, hidden_width, piece):
            part = slice(first, first + piece)
            gate = jnp.dot(arrived, gate_ref[:, part], preferred_element_type=jnp.float32)
            upper = jnp.dot(arrived, up_ref[:, part], preferred_element_type=jnp.float32)
            hidden.append((jax.nn.silu(gate) * upper).astype(jnp.bfloat16))
        hidden = jnp.concatenate(hidden, axis=1)
        for first in range(0, width, piece):
            part = slice(first, first + piece)
            result = jnp.dot(hidden, down_ref[:, part], preferred_element_type=jnp.float32)
            outbox[pl.ds(pair * 2, 2), :, part] = result.astype(jnp.bfloat16).reshape(
                2, capacity, piece
            )

        @pl.when(pair > 0)
        def _():
            home(pair * 2).start()

        @pl.when(pair == 0)
        def _():
            back[0] = outbox[0]

        home(pair * 2 + 1).start()

    total[...] = stream_ref[...].astype(jnp.float32)

    @pl.loop(0, pairs)
    def _(step):
        pair = lax.rem(pairs - step, pairs)

        @pl.when(pair > 0)
        def _():
            home(pair * 2).wait_recv()

        home(pair * 2 + 1).wait_recv()
        slot = lax.broadcasted_iota(jnp.int32, (rows, 2 * capacity), 1)
        even, odd = flipped(me, pair * 2, n), flipped(me, pair * 2 + 1, n)
        slot = jnp.where(slot < capacity, slot + even * capacity, slot - capacity + odd * capacity)
        first = (target_ref[:, 0:1] == slot).astype(jnp.bfloat16)
        second = (target_ref[:, 1:2] == slot).astype(jnp.bfloat16)
        for start in range(0, width, piece):
            part = slice(start, start + piece)
            block = back[pl.ds(pair * 2, 2), :, part].reshape(2 * capacity, piece)
            total[:, part] += share_ref[:, 0:1] * jnp.dot(
                first, block, preferred_element_type=jnp.float32
            ) + share_ref[:, 1:2] * jnp.dot(second, block, preferred_element_type=jnp.float32)

    out_ref[...] = total[...].astype(jnp.bfloat16)

    @pl.loop(1, n)
    def _(off):
        there(off).wait_send()
        home(off).wait_send()


def experts(normed, stream, target, share, w_gate, w_up, w_down):
    n = lax.axis_size("sp")
    rows, width = normed.shape
    capacity = 4 * rows // n
    hidden = w_gate.shape[2]
    bf16 = jnp.bfloat16
    vmem = pl.BlockSpec(memory_space=pltpu.VMEM)
    return pl.pallas_call(
        functools.partial(expert_kernel, n),
        out_shape=jax.ShapeDtypeStruct((rows, width), bf16),
        in_specs=[vmem] * 5 + [pl.BlockSpec(memory_space=pl.ANY)] * 3,
        out_specs=vmem,
        scratch_shapes=[
            pltpu.VMEM((width, hidden), bf16),
            pltpu.VMEM((width, hidden), bf16),
            pltpu.VMEM((hidden, width), bf16),
            pltpu.VMEM((n, capacity, width), bf16),
            pltpu.VMEM((n, capacity, width), bf16),
            pltpu.VMEM((n, capacity, width), bf16),
            pltpu.VMEM((n, capacity, width), bf16),
            pltpu.VMEM((rows, width), jnp.float32),
            pltpu.SemaphoreType.DMA((3,)),
            pltpu.SemaphoreType.DMA((n,)),
            pltpu.SemaphoreType.DMA((n,)),
            pltpu.SemaphoreType.DMA((n,)),
            pltpu.SemaphoreType.DMA((n,)),
        ],
        compiler_params=pltpu.CompilerParams(
            collective_id=1, has_side_effects=True, vmem_limit_bytes=50 * 1024 * 1024
        ),
    )(normed, stream, target, target.T, share, w_gate, w_up, w_down)


def body(
    queries,
    keys,
    values,
    proj_weight,
    residual,
    norm_gain,
    route,
    route_weight,
    w_gate,
    w_up,
    w_down,
):
    seq_span = lax.axis_size("sp")
    rows = queries.shape[1]
    width = queries.shape[2]
    stream, normed = attention(
        queries[0], keys[0], values[0], proj_weight, residual[0], norm_gain
    )
    capacity = 4 * rows // seq_span
    chosen = route[0].reshape(rows * 2)
    one_hot = (chosen[:, None] == jnp.arange(seq_span, dtype=jnp.int32)[None, :]).astype(jnp.int32)
    earlier = jnp.cumsum(one_hot, axis=0) - one_hot
    slot = jnp.sum(earlier * one_hot, axis=1)
    target = (chosen * capacity + slot).reshape(rows, 2)
    return experts(normed, stream, target, route_weight[0], w_gate, w_up, w_down)[None]


def solution(mesh):
    return jax.shard_map(
        body,
        mesh=mesh,
        in_specs=(
            P("dp", "sp", None),
            P("dp", "sp", None),
            P("dp", "sp", None),
            P("sp", None),
            P("dp", "sp", None),
            P(),
            P("dp", "sp", None),
            P("dp", "sp", None),
            P("sp", None, None),
            P("sp", None, None),
            P("sp", None, None),
        ),
        out_specs=P("dp", "sp", None),
        check_vma=False,
    )
```
